32 devices in a mesh: sp: 8 (over z, y), dp: 4 (over x, core).
Axes of the slice: x: 2, y: 2, z: 4, core: 2. Of those that a mesh axis runs over, the one named last changes fastest.
Arguments:
- out_cotangent: bfloat16 [4, 2048, 2048], P('dp', 'sp'), may hold values from -6 to 6
- value_pre: bfloat16 [4, 2048, 2048], P('dp', 'sp'), may hold values from -8 to 8
- gate_pre: bfloat16 [4, 2048, 2048], P('dp', 'sp'), may hold values from -8 to 8
- out_weight: bfloat16 [2048, 2048], P('dp'), may hold values from -0.125 to 0.125
- conv_kernel: bfloat16 [31, 2048], P(None, 'sp'), may hold values from -6 to 6
- norm_gain: bfloat16 [2048], P('sp'), may hold values from 0.099609375 to 1.8984375
Outputs:
- grad_value: bfloat16 [4, 2048, 2048], P('dp', 'sp')
- grad_gate: bfloat16 [4, 2048, 2048], P('dp', 'sp')
- grad_out_weight: float32 [2048, 2048], P(('sp', 'dp'))
- grad_kernel: float32 [31, 2048], P(None, 'sp')
- grad_gain: float32 [2048], P('sp')
The draws below stay inside these ranges and needn't reach their ends.
All inputs are finite; a program needn't handle non-finite values.
Results may differ from the reference program's by a relative error of at most 0.011.
Values may be sent and summed in bfloat16 or wider, within the bound.
A program may use at most 128 MiB of HBM per device.

```python
import math
import jax
import jax.numpy as jnp
from jax import lax

D = 2048
CONV_W = 31
SEQS = 4
LENGTH = 2048
TOKENS = 8192


def draw_value_pre(key, part):
    keys = jax.random.split(jax.random.fold_in(key, 11), 2)
    shape = (SEQS, LENGTH, D)
    row_scale = jnp.exp(jax.random.uniform(keys[1], (SEQS, LENGTH, 1), jnp.float32, math.log(0.4), math.log(2.5)))
    values_out = jax.random.normal(keys[0], shape, jnp.float32) * row_scale
    return jnp.clip(values_out, -8.0, 8.0).astype(jnp.bfloat16)


def draw_conv_kernel(key, part):
    keys = jax.random.split(jax.random.fold_in(key, 23), 2)
    position = jnp.arange(D, dtype=jnp.float32) / float(D)
    rough = jnp.exp(jax.random.uniform(keys[1], (1, D), jnp.float32, math.log(0.5), math.log(2.0)))
    column_scale = jnp.exp(math.log(6.0) * position)[None, :] * rough
    taps = jax.random.normal(keys[0], (CONV_W, D), jnp.float32)
    taps = taps * column_scale * float(CONV_W) ** (-0.5)
    return jnp.clip(taps, -6.0, 6.0).astype(jnp.bfloat16)


def shard_levels(rng, shape, pieces, low, high):
    def one(axis_at, blocks):
        steps = jax.random.uniform(jax.random.fold_in(jax.random.fold_in(rng, 6), axis_at), (blocks,), jnp.float32, low / len(pieces), high / len(pieces))
        return jnp.repeat(jnp.exp(steps), shape[axis_at] // blocks).reshape((-1,) + (1,) * (len(shape) - axis_at - 1))

    gain = one(*pieces[0])
    for cut in pieces[1:]:
        gain = gain * one(*cut)
    return gain


def normal_values(rng, shape, spread, limit, cuts=(), kind=jnp.bfloat16):
    values = jax.random.normal(rng, shape, jnp.float32) * spread
    if len(cuts) > 0:
        values = shard_levels(rng, shape, cuts, -0.22, 0.18) * values
    return jnp.clip(values, min=-limit, max=limit).astype(kind)


def setup_inputs(seed: int = 0) -> dict:
    key_list = jax.random.split(jax.random.key(seed), 7)
    out_cotangent = normal_values(key_list[0], (SEQS, LENGTH, D), 1.0, 6.0, ((0, 4), (1, 8)))
    value_pre = draw_value_pre(jax.random.fold_in(key_list[6], 71), 0)
    gate_pre = normal_values(key_list[2], (SEQS, LENGTH, D), 1.5, 8.0, ((0, 4), (1, 8)))
    out_weight = normal_values(key_list[3], (D, D), D ** -0.5, 0.125, ((0, 4),))
    conv_kernel = draw_conv_kernel(jax.random.fold_in(key_list[6], 71), 0)
    norm_gain = jnp.clip(1.0 + 0.18 * jax.random.normal(key_list[5], (D,), jnp.float32), 0.099609375, 1.8984375).astype(jnp.bfloat16)
    return {"out_cotangent": out_cotangent, "value_pre": value_pre, "gate_pre": gate_pre, "out_weight": out_weight, "conv_kernel": conv_kernel, "norm_gain": norm_gain}


epsilon = 1e-05

def shift_down(array, offset):
    return jnp.pad(array, ((offset, 0), (0, 0)))[:array.shape[0]]

def shift_up(array, offset):
    return jnp.pad(array, ((0, offset), (0, 0)))[offset:]

def reference(out_cotangent, value_pre, gate_pre, out_weight, conv_kernel, norm_gain):
    taps_float = conv_kernel.astype(jnp.float32)
    gain_float = norm_gain.astype(jnp.float32)
    weight_sum = jnp.zeros((D, D), jnp.float32)
    kernel_sum = jnp.zeros((CONV_W, D), jnp.float32)
    gain_sum = jnp.zeros((D,), jnp.float32)
    value_grads = []
    gate_grads = []
    for sequence in range(SEQS):
        cotangent = out_cotangent[sequence]
        values_in = value_pre[sequence].astype(jnp.float32)
        sigmoid_gate = jax.nn.sigmoid(gate_pre[sequence].astype(jnp.float32))
        gated = (values_in * sigmoid_gate).astype(jnp.bfloat16)
        gated_float = gated.astype(jnp.float32)
        conv = jnp.zeros(gated_float.shape, jnp.float32)
        for offset in range(CONV_W):
            conv = conv + taps_float[offset] * shift_down(gated_float, offset)
        centre = lax.optimization_barrier(jnp.mean(conv, axis=1, keepdims=True))
        deviation = conv - centre
        variance = lax.optimization_barrier(jnp.mean(deviation * deviation, axis=1, keepdims=True))
        inv_scale = lax.rsqrt(variance + epsilon)
        centred = deviation * inv_scale
        normed = centred * gain_float
        activation = jax.nn.silu(normed).astype(jnp.bfloat16)
        grad_act = lax.dot_general(cotangent, out_weight, (((1,), (1,)), ((), ())), preferred_element_type=jnp.float32).astype(jnp.bfloat16)
        weight_sum = weight_sum + lax.dot_general(activation, cotangent, (((0,), (0,)), ((), ())), preferred_element_type=jnp.float32)
        sig_norm = jax.nn.sigmoid(normed)
        grad_normed = grad_act.astype(jnp.float32) * sig_norm * (1.0 + normed * (1.0 - sig_norm))
        gain_sum = gain_sum + lax.optimization_barrier(jnp.sum(grad_normed * centred, axis=0))
        grad_centred = grad_normed * gain_float
        grad_conv = (grad_centred - lax.optimization_barrier(jnp.mean(grad_centred, axis=1, keepdims=True)) - centred * lax.optimization_barrier(jnp.mean(grad_centred * centred, axis=1, keepdims=True))) * inv_scale
        kernel_rows = [lax.optimization_barrier(jnp.sum(grad_conv * shift_down(gated_float, offset), axis=0)) for offset in range(CONV_W)]
        kernel_sum = kernel_sum + jnp.stack(kernel_rows, axis=0)
        grad_gated = jnp.zeros(grad_conv.shape, jnp.float32)
        for offset in range(CONV_W):
            grad_gated = grad_gated + taps_float[offset] * shift_up(grad_conv, offset)
        grad_gated = grad_gated.astype(jnp.bfloat16).astype(jnp.float32)
        value_grads.append((grad_gated * sigmoid_gate).astype(jnp.bfloat16))
        gate_grads.append((grad_gated * values_in * sigmoid_gate * (1.0 - sigmoid_gate)).astype(jnp.bfloat16))
    factor = float(TOKENS) ** (-0.5)
    return (jnp.stack(value_grads, axis=0), jnp.stack(gate_grads, axis=0), weight_sum * factor, kernel_sum * factor, gain_sum * factor)
```

```python
import functools

import jax
import jax.numpy as jnp
from jax import lax
from jax.experimental import pallas as pl
from jax.experimental.pallas import tpu as pltpu
from jax.sharding import PartitionSpec as P

epsilon = 1e-05
LANES = 128
HALVES = 2
f32 = jnp.float32
bf16 = jnp.bfloat16


def block_kernel(
    S, N, T, C, K, HB, ids,
    cot, val, gate, w, taps,
    gv, gg, gw, kout,
    cot_all, ext, cen, gc, gext, kall, act, act_all, ga_send, ga, wpart, rbuf,
    kg, krecv, ksum, k2recv, send_sem, recv_sem,
):
    s = lax.axis_index("sp")
    d = lax.axis_index("dp")
    chunks = C // LANES
    cps = chunks // S
    cpd = chunks // N
    block = C // (S * N)
    RB = min(T, 128)
    total = S * N
    me = s * N + d
    partner = d + 1 - 2 * lax.rem(d, 2)
    factor = float(S * N * T) ** (-0.5)
    hrows = T // HALVES
    waits = []

    def copy(src, dst, i, to_s, to_d):
        return pltpu.make_async_remote_copy(
            src_ref=src, dst_ref=dst, send_sem=send_sem.at[i], recv_sem=recv_sem.at[i],
            device_id={"sp": to_s, "dp": to_d}, device_id_type=pl.DeviceIdType.MESH,
        )

    def send(src, dst, i, to_s, to_d):
        c = copy(src, dst, i, to_s, to_d)
        c.start()
        waits.append(c)

    def arrived(dst, i):
        copy(dst, dst, i, s, partner).wait_recv()

    barrier = pltpu.get_barrier_semaphore()

    def greet(j, _):
        other = lax.rem(me + j, total)
        pl.semaphore_signal(
            barrier, inc=1, device_id={"sp": other // N, "dp": lax.rem(other, N)},
            device_id_type=pl.DeviceIdType.MESH,
        )
        return _

    lax.fori_loop(1, total, greet, 0)
    def gate_chunk(cb, _):
        cols = pl.ds(pl.multiple_of(cb * LANES, LANES), LANES)
        sig = jax.nn.sigmoid(gate[:, cols].astype(f32))
        ext[cb, pl.ds(HB, T), :] = (val[:, cols].astype(f32) * sig).astype(bf16).astype(f32)
        return _

    lax.fori_loop(0, chunks, gate_chunk, 0)
    pl.semaphore_wait(barrier, total - 1)

    for j in range(1, S):
        send(taps, kall.at[pl.ds(s * cps, cps)], ids["taps"] + j, lax.rem(s + j, S), d)
    following = lax.rem(s + 1, S)
    preceding = lax.rem(s + S - 1, S)
    send(ext.at[:, pl.ds(T, HB), :], ext.at[:, pl.ds(0, HB), :], ids["front"], following, d)
    for j in range(1, N // 2):
        for h in range(HALVES):
            rows = pl.ds(h * hrows, hrows)
            send(cot.at[rows], cot_all.at[d, rows], ids["mirror"] + j * HALVES + h, s, lax.rem(d + 2 * j, N))
    send(cot, cot_all.at[d], ids["partner"], s, partner)
    kall[pl.ds(s * cps, cps)] = taps[...]
    cot_all[d] = cot[...]
    for j in range(1, S):
        arrived(kall.at[pl.ds(lax.rem(s + S - j, S) * cps, cps)], ids["taps"] + j)
    arrived(ext.at[:, pl.ds(0, HB), :], ids["front"])

    @pl.when(s == 0)
    def _():
        ext[:, pl.ds(0, HB), :] = jnp.zeros((chunks, HB, LANES), f32)

    def conv_chunk(cb, sums):
        tf = kall[cb].astype(f32)
        parts = []
        for rb in range(T // RB):
            acc = jnp.zeros((RB, LANES), f32)
            for k in range(K):
                acc = acc + tf[k : k + 1] * ext[cb, pl.ds(HB - k + rb * RB, RB), :]
            cen[cb, pl.ds(rb * RB, RB), :] = acc
            parts.append(jnp.sum(acc, axis=1, keepdims=True))
        return sums + jnp.concatenate(parts, axis=0)

    column = jnp.zeros((T, 1), f32)
    mean = lax.fori_loop(0, chunks, conv_chunk, column) / C

    def square_chunk(cb, sums):
        dev = cen[cb] - mean
        return sums + dev * dev

    squares = lax.fori_loop(0, chunks, square_chunk, jnp.zeros((T, LANES), f32))
    inv = lax.rsqrt(jnp.sum(squares, axis=1, keepdims=True) / C + epsilon)

    def relay():
        for j in range(1, N // 2):
            origin = lax.rem(d + N - 2 * j, N)
            for h in range(HALVES):
                piece = cot_all.at[origin, pl.ds(h * hrows, hrows)]
                arrived(piece, ids["mirror"] + j * HALVES + h)
                send(piece, piece, ids["relay"] + j * HALVES + h, s, partner)

    def act_chunk(cb, _):
        centred = (cen[cb] - mean) * inv
        cen[cb] = centred
        normed = centred * kall[cb].astype(f32)[K : K + 1]
        act[cb] = (normed * jax.nn.sigmoid(normed)).astype(bf16)
        return _

    lax.fori_loop(0, chunks, act_chunk, 0)
    for j in range(1, N):
        to = lax.rem(d + j, N)
        send(act.at[pl.ds(to * cpd, cpd)], act_all.at[d], ids["act"] + j, s, to)
    act_all[d] = act[pl.ds(d * cpd, cpd)]

    def project(source, slot):
        def pair(m, _):
            rows = pl.ds(pl.multiple_of(m * 2 * LANES, 2 * LANES), 2 * LANES)
            out = lax.dot_general(
                cot_all[source], w[rows, :], (((1,), (1,)), ((), ())), preferred_element_type=f32
            ).astype(bf16)
            ga_send[slot, 2 * m] = out[:, :LANES]
            ga_send[slot, 2 * m + 1] = out[:, LANES:]
            return _

        lax.fori_loop(0, cpd // 2, pair, 0)

    mine = pl.ds(d * cpd, cpd)
    project(d, 0)
    ga[mine] = ga_send[0]
    arrived(cot_all.at[partner], ids["partner"])
    project(partner, 1)
    send(ga_send.at[1], ga.at[mine], ids["ga"] + 1, s, partner)
    relay()
    for j in range(1, N // 2):
        origin = lax.rem(d + N - 2 * j, N)
        project(origin, 2 * j)
        send(ga_send.at[2 * j], ga.at[mine], ids["ga"] + 2 * j, s, origin)
    for j in range(1, N // 2):
        origin = lax.rem(partner + N - 2 * j, N)
        for h in range(HALVES):
            arrived(cot_all.at[origin, pl.ds(h * hrows, hrows)], ids["relay"] + j * HALVES + h)
        project(origin, 2 * j + 1)
        send(ga_send.at[2 * j + 1], ga.at[mine], ids["ga"] + 2 * j + 1, s, origin)

    for j in range(1, N):
        arrived(act_all.at[lax.rem(d + N - j, N)], ids["act"] + j)
    NT = min(C, 512)

    def weight_tile(i, _):
        m, n = i // (C // NT), lax.rem(i, C // NT)
        cols = pl.ds(pl.multiple_of(n * NT, NT), NT)
        acc = jnp.zeros((LANES, NT), f32)
        for q in range(N):
            acc = acc + lax.dot_general(
                act_all[q, m], cot_all[q, :, cols], (((0,), (0,)), ((), ())),
                preferred_element_type=f32,
            )
        wpart[pl.ds(pl.multiple_of(m * LANES, LANES), LANES), cols] = acc.astype(bf16)
        return _

    lax.fori_loop(0, cpd * (C // NT), weight_tile, 0)

    def block_of(j):
        i = lax.rem(s + j, S)
        owner = d * S + i
        rows = pl.ds(pl.multiple_of(i * block, block), block)
        return owner, rows, pltpu.make_async_remote_copy(
            src_ref=wpart.at[rows], dst_ref=rbuf.at[s], send_sem=send_sem.at[ids["rs"] + j],
            recv_sem=recv_sem.at[ids["rs"] + s],
            device_id={"sp": owner // N, "dp": lax.rem(owner, N)},
            device_id_type=pl.DeviceIdType.MESH,
        )

    for j in range(S):
        owner, rows, c = block_of(j)

        @pl.when(owner != me)
        def _():
            c.start()

        @pl.when(owner == me)
        def _():
            rbuf[s] = wpart[rows, :]

    for j in range(1, N // 2):
        arrived(ga.at[pl.ds(lax.rem(d + 2 * j, N) * cpd, cpd)], ids["ga"] + 2 * j)
        arrived(ga.at[pl.ds(lax.rem(partner + 2 * j, N) * cpd, cpd)], ids["ga"] + 2 * j + 1)
    arrived(ga.at[pl.ds(partner * cpd, cpd)], ids["ga"] + 1)

    def grad_chunk(cb, sums):
        one, two = sums
        centred = cen[cb]
        gain = kall[cb].astype(f32)[K : K + 1]
        normed = centred * gain
        sg = jax.nn.sigmoid(normed)
        grad = ga[cb].astype(f32) * sg * (1.0 + normed * (1.0 - sg))
        kg[cb, pl.ds(K, 1), :] = jnp.sum(grad * centred, axis=0, keepdims=True)
        grad = grad * gain
        gc[cb] = grad
        return one + grad, two + grad * centred

    zero = jnp.zeros((T, LANES), f32)
    one, two = lax.fori_loop(0, chunks, grad_chunk, (zero, zero))
    first = jnp.sum(one, axis=1, keepdims=True) / C
    second = jnp.sum(two, axis=1, keepdims=True) / C

    def conv_grad(cb, _):
        gext[cb, pl.ds(0, T), :] = (gc[cb] - first - cen[cb] * second) * inv
        return _

    lax.fori_loop(0, chunks, conv_grad, 0)
    send(gext.at[:, pl.ds(0, HB), :], gext.at[:, pl.ds(T, HB), :], ids["back"], preceding, d)

    def taps_chunk(cb, _):
        for k in range(K):
            acc = jnp.zeros((8, LANES), f32)
            for rb in range(T // RB):
                prod = gext[cb, pl.ds(rb * RB, RB), :] * ext[cb, pl.ds(HB - k + rb * RB, RB), :]
                acc = acc + jnp.sum(prod.reshape(RB // 8, 8, LANES), axis=0)
            kg[cb, pl.ds(k, 1), :] = jnp.sum(acc, axis=0, keepdims=True)
        return _

    lax.fori_loop(0, chunks, taps_chunk, 0)
    for j in range(1, S):
        to = lax.rem(s + j, S)
        send(kg.at[pl.ds(to * cps, cps)], krecv.at[j], ids["kg"] + j, to, d)

    arrived(gext.at[:, pl.ds(T, HB), :], ids["back"])

    @pl.when(s == S - 1)
    def _():
        gext[:, pl.ds(T, HB), :] = jnp.zeros((chunks, HB, LANES), f32)

    def gated_chunk(cb, _):
        cols = pl.ds(pl.multiple_of(cb * LANES, LANES), LANES)
        tf = kall[cb].astype(f32)
        for rb in range(T // RB):
            rows = pl.ds(rb * RB, RB)
            acc = jnp.zeros((RB, LANES), f32)
            for k in range(K):
                acc = acc + tf[k : k + 1] * gext[cb, pl.ds(k + rb * RB, RB), :]
            acc = acc.astype(bf16).astype(f32)
            sig = jax.nn.sigmoid(gate[rows, cols].astype(f32))
            gv[rows, cols] = (acc * sig).astype(bf16)
            gg[rows, cols] = (acc * val[rows, cols].astype(f32) * sig * (1.0 - sig)).astype(bf16)
        return _

    lax.fori_loop(0, chunks, gated_chunk, 0)

    acc = kg[pl.ds(s * cps, cps)]
    for j in range(1, S):
        arrived(krecv.at[j], ids["kg"] + j)
        acc = acc + krecv[j]
    ksum[...] = acc
    for j in range(1, N):
        send(ksum, k2recv.at[j], ids["k2"] + j, s, lax.rem(d + j, N))
    for j in range(1, N):
        arrived(k2recv.at[j], ids["k2"] + j)
        acc = acc + k2recv[j]
    kout[...] = acc * factor

    home = me // S
    for q in range(S):
        @pl.when(jnp.logical_or(q != s, home != d))
        def _():
            arrived(rbuf.at[q], ids["rs"] + q)

    def sum_tile(n, _):
        cols = pl.ds(pl.multiple_of(n * LANES, LANES), LANES)
        acc = rbuf[0, :, cols].astype(f32)
        for q in range(1, S):
            acc = acc + rbuf[q, :, cols].astype(f32)
        gw[:, cols] = acc * factor
        return _

    lax.fori_loop(0, chunks, sum_tile, 0)
    for j in range(S):
        owner, rows, c = block_of(j)

        @pl.when(owner != me)
        def _():
            c.wait_send()

    for c in waits:
        c.wait_send()


def shards(out_cotangent, value_pre, gate_pre, out_weight, conv_kernel, norm_gain):
    S, N = lax.axis_size("sp"), lax.axis_size("dp")
    _, T, C = out_cotangent.shape
    K = conv_kernel.shape[0]
    chunks, cps, cpd, block = C // LANES, C // LANES // S, C // LANES // N, C // (S * N)
    HB = -(-(K - 1) // 16) * 16
    KP = -(-(K + 1) // 16) * 16
    packed = jnp.concatenate(
        [conv_kernel, norm_gain[None], jnp.zeros((KP - K - 1, C // S), bf16)], axis=0
    )
    packed = jnp.transpose(packed.reshape(KP, cps, LANES), (1, 0, 2))
    ids, count = {}, 0
    for name, size in (
        ("taps", S), ("front", 1), ("back", 1), ("partner", 1), ("mirror", N // 2 * HALVES),
        ("relay", N // 2 * HALVES), ("act", N), ("ga", N), ("rs", S), ("kg", S), ("k2", N),
    ):
        ids[name] = count
        count += size
    vm = pl.BlockSpec(memory_space=pltpu.VMEM)
    grad_value, grad_gate, grad_weight, small = pl.pallas_call(
        functools.partial(block_kernel, S, N, T, C, K, HB, ids),
        out_shape=(
            jax.ShapeDtypeStruct((T, C), bf16),
            jax.ShapeDtypeStruct((T, C), bf16),
            jax.ShapeDtypeStruct((block, C), f32),
            jax.ShapeDtypeStruct((cps, KP, LANES), f32),
        ),
        in_specs=[vm] * 5,
        out_specs=(vm,) * 4,
        scratch_shapes=[
            pltpu.VMEM((N, T, C), bf16),
            pltpu.VMEM((chunks, T + HB, LANES), f32),
            pltpu.VMEM((chunks, T, LANES), f32),
            pltpu.VMEM((chunks, T, LANES), f32),
            pltpu.VMEM((chunks, T + HB, LANES), f32),
            pltpu.VMEM((chunks, KP, LANES), bf16),
            pltpu.VMEM((chunks, T, LANES), bf16),
            pltpu.VMEM((N, cpd, T, LANES), bf16),
            pltpu.VMEM((N, cpd, T, LANES), bf16),
            pltpu.VMEM((chunks, T, LANES), bf16),
            pltpu.VMEM((cpd * LANES, C), bf16),
            pltpu.VMEM((S, block, C), bf16),
            pltpu.VMEM((chunks, KP, LANES), f32),
            pltpu.VMEM((S, cps, KP, LANES), f32),
            pltpu.VMEM((cps, KP, LANES), f32),
            pltpu.VMEM((N, cps, KP, LANES), f32),
            pltpu.SemaphoreType.DMA((count,)),
            pltpu.SemaphoreType.DMA((count,)),
        ],
        compiler_params=pltpu.CompilerParams(
            collective_id=0, has_side_effects=True, vmem_limit_bytes=60 * 1024 * 1024
        ),
        name="block_backward",
    )(out_cotangent[0], value_pre[0], gate_pre[0], out_weight, packed)
    small = jnp.transpose(small, (1, 0, 2)).reshape(KP, C // S)
    return grad_value[None], grad_gate[None], grad_weight, small[:K], small[K]


def solution(mesh):
    placed = (
        P("dp", "sp", None),
        P("dp", "sp", None),
        P("dp", "sp", None),
        P("dp", None),
        P(None, "sp"),
        P("sp"),
    )
    return jax.shard_map(
        shards,
        mesh=mesh,
        in_specs=placed,
        out_specs=(
            P("dp", "sp", None),
            P("dp", "sp", None),
            P(("sp", "dp"), None),
            P(None, "sp"),
            P("sp"),
        ),
        check_vma=False,
    )
```

```python
import functools

import jax
import jax.numpy as jnp
from jax import lax
from jax.experimental import pallas as pl
from jax.experimental.pallas import tpu as pltpu
from jax.sharding import PartitionSpec as P

epsilon = 1e-05
LANES = 128
HALVES = 2
f32 = jnp.float32
bf16 = jnp.bfloat16


def block_kernel(
    S, N, T, C, K, HB, ids,
    cot, val, gate, w, taps,
    gv, gg, gw, kout, gout,
    cot_all, ext, cen, gc, gext, kall, act, act_all, ga_send, ga, wpart, rbuf,
    kg, krecv, ksum, k2recv, send_sem, recv_sem,
):
    s = lax.axis_index("sp")
    d = lax.axis_index("dp")
    chunks = C // LANES
    cps = chunks // S
    cpd = chunks // N
    block = C // (S * N)
    RB = min(T, 128)
    total = S * N
    me = s * N + d
    partner = d + 1 - 2 * lax.rem(d, 2)
    factor = float(S * N * T) ** (-0.5)
    hrows = T // HALVES
    waits = []

    def copy(src, dst, i, to_s, to_d):
        return pltpu.make_async_remote_copy(
            src_ref=src, dst_ref=dst, send_sem=send_sem.at[i], recv_sem=recv_sem.at[i],
            device_id={"sp": to_s, "dp": to_d}, device_id_type=pl.DeviceIdType.MESH,
        )

    def send(src, dst, i, to_s, to_d):
        c = copy(src, dst, i, to_s, to_d)
        c.start()
        waits.append(c)

    def arrived(dst, i):
        copy(dst, dst, i, s, partner).wait_recv()

    barrier = pltpu.get_barrier_semaphore()

    def greet(j, _):
        other = lax.rem(me + j, total)
        pl.semaphore_signal(
            barrier, inc=1, device_id={"sp": other // N, "dp": lax.rem(other, N)},
            device_id_type=pl.DeviceIdType.MESH,
        )
        return _

    lax.fori_loop(1, total, greet, 0)
    def gate_chunk(cb, _):
        cols = pl.ds(pl.multiple_of(cb * LANES, LANES), LANES)
        sig = jax.nn.sigmoid(gate[:, cols].astype(f32))
        ext[cb, pl.ds(HB, T), :] = (val[:, cols].astype(f32) * sig).astype(bf16).astype(f32)
        return _

    lax.fori_loop(0, chunks, gate_chunk, 0)
    pl.semaphore_wait(barrier, total - 1)

    for j in range(1, S):
        send(taps, kall.at[pl.ds(s * cps, cps)], ids["taps"] + j, lax.rem(s + j, S), d)
    following = lax.rem(s + 1, S)
    preceding = lax.rem(s + S - 1, S)
    send(ext.at[:, pl.ds(T, HB), :], ext.at[:, pl.ds(0, HB), :], ids["front"], following, d)
    for j in range(1, N // 2):
        for h in range(HALVES):
            rows = pl.ds(h * hrows, hrows)
            send(cot.at[rows], cot_all.at[d, rows], ids["mirror"] + j * HALVES + h, s, lax.rem(d + 2 * j, N))
    send(cot, cot_all.at[d], ids["partner"], s, partner)
    kall[pl.ds(s * cps, cps)] = taps[...]
    cot_all[d] = cot[...]
    for j in range(1, S):
        arrived(kall.at[pl.ds(lax.rem(s + S - j, S) * cps, cps)], ids["taps"] + j)
    arrived(ext.at[:, pl.ds(0, HB), :], ids["front"])

    @pl.when(s == 0)
    def _():
        ext[:, pl.ds(0, HB), :] = jnp.zeros((chunks, HB, LANES), f32)

    def conv_chunk(cb, sums):
        tf = kall[cb].astype(f32)
        parts = []
        for rb in range(T // RB):
            acc = jnp.zeros((RB, LANES), f32)
            for k in range(K):
                acc = acc + tf[k : k + 1] * ext[cb, pl.ds(HB - k + rb * RB, RB), :]
            cen[cb, pl.ds(rb * RB, RB), :] = acc
            parts.append(jnp.sum(acc, axis=1, keepdims=True))
        return sums + jnp.concatenate(parts, axis=0)

    column = jnp.zeros((T, 1), f32)
    mean = lax.fori_loop(0, chunks, conv_chunk, column) / C

    def square_chunk(cb, sums):
        dev = cen[cb] - mean
        return sums + dev * dev

    squares = lax.fori_loop(0, chunks, square_chunk, jnp.zeros((T, LANES), f32))
    inv = lax.rsqrt(jnp.sum(squares, axis=1, keepdims=True) / C + epsilon)

    def relay():
        for j in range(1, N // 2):
            origin = lax.rem(d + N - 2 * j, N)
            for h in range(HALVES):
                piece = cot_all.at[origin, pl.ds(h * hrows, hrows)]
                arrived(piece, ids["mirror"] + j * HALVES + h)
                send(piece, piece, ids["relay"] + j * HALVES + h, s, partner)

    def act_chunk(cb, _):
        centred = (cen[cb] - mean) * inv
        cen[cb] = centred
        normed = centred * kall[cb].astype(f32)[K : K + 1]
        act[cb] = (normed * jax.nn.sigmoid(normed)).astype(bf16)
        return _

    lax.fori_loop(0, chunks, act_chunk, 0)
    for j in range(1, N):
        to = lax.rem(d + j, N)
        send(act.at[pl.ds(to * cpd, cpd)], act_all.at[d], ids["act"] + j, s, to)
    act_all[d] = act[pl.ds(d * cpd, cpd)]

    def project(source, slot):
        def pair(m, _):
            rows = pl.ds(pl.multiple_of(m * 2 * LANES, 2 * LANES), 2 * LANES)
            out = lax.dot_general(
                cot_all[source], w[rows, :], (((1,), (1,)), ((), ())), preferred_element_type=f32
            ).astype(bf16)
            ga_send[slot, 2 * m] = out[:, :LANES]
            ga_send[slot, 2 * m + 1] = out[:, LANES:]
            return _

        lax.fori_loop(0, cpd // 2, pair, 0)

    mine = pl.ds(d * cpd, cpd)
    project(d, 0)
    ga[mine] = ga_send[0]
    arrived(cot_all.at[partner], ids["partner"])
    project(partner, 1)
    send(ga_send.at[1], ga.at[mine], ids["ga"] + 1, s, partner)
    relay()
    for j in range(1, N // 2):
        origin = lax.rem(d + N - 2 * j, N)
        project(origin, 2 * j)
        send(ga_send.at[2 * j], ga.at[mine], ids["ga"] + 2 * j, s, origin)
    for j in range(1, N // 2):
        origin = lax.rem(partner + N - 2 * j, N)
        for h in range(HALVES):
            arrived(cot_all.at[origin, pl.ds(h * hrows, hrows)], ids["relay"] + j * HALVES + h)
        project(origin, 2 * j + 1)
        send(ga_send.at[2 * j + 1], ga.at[mine], ids["ga"] + 2 * j + 1, s, origin)

    for j in range(1, N):
        arrived(act_all.at[lax.rem(d + N - j, N)], ids["act"] + j)
    NT = min(C, 512)

    def weight_tile(i, _):
        m, n = i // (C // NT), lax.rem(i, C // NT)
        cols = pl.ds(pl.multiple_of(n * NT, NT), NT)
        acc = jnp.zeros((LANES, NT), f32)
        for q in range(N):
            acc = acc + lax.dot_general(
                act_all[q, m], cot_all[q, :, cols], (((0,), (0,)), ((), ())),
                preferred_element_type=f32,
            )
        wpart[pl.ds(pl.multiple_of(m * LANES, LANES), LANES), cols] = acc.astype(bf16)
        return _

    lax.fori_loop(0, cpd * (C // NT), weight_tile, 0)

    def block_of(j):
        i = lax.rem(s + j, S)
        owner = d * S + i
        rows = pl.ds(pl.multiple_of(i * block, block), block)
        return owner, rows, pltpu.make_async_remote_copy(
            src_ref=wpart.at[rows], dst_ref=rbuf.at[s], send_sem=send_sem.at[ids["rs"] + j],
            recv_sem=recv_sem.at[ids["rs"] + s],
            device_id={"sp": owner // N, "dp": lax.rem(owner, N)},
            device_id_type=pl.DeviceIdType.MESH,
        )

    def send_blocks(first, last):
        for j in range(first, last):
            owner, rows, c = block_of(j)

            @pl.when(owner != me)
            def _():
                c.start()

            @pl.when(owner == me)
            def _():
                rbuf[s] = wpart[rows, :]

    send_blocks(0, S // 2)

    for j in range(1, N // 2):
        arrived(ga.at[pl.ds(lax.rem(d + 2 * j, N) * cpd, cpd)], ids["ga"] + 2 * j)
        arrived(ga.at[pl.ds(lax.rem(partner + 2 * j, N) * cpd, cpd)], ids["ga"] + 2 * j + 1)
    arrived(ga.at[pl.ds(partner * cpd, cpd)], ids["ga"] + 1)

    def grad_chunk(cb, sums):
        one, two = sums
        centred = cen[cb]
        gain = kall[cb].astype(f32)[K : K + 1]
        normed = centred * gain
        sg = jax.nn.sigmoid(normed)
        grad = ga[cb].astype(f32) * sg * (1.0 + normed * (1.0 - sg))
        kg[cb, pl.ds(K, 1), :] = jnp.sum(grad * centred, axis=0, keepdims=True)
        grad = grad * gain
        gc[cb] = grad
        return one + grad, two + grad * centred

    zero = jnp.zeros((T, LANES), f32)
    one, two = lax.fori_loop(0, chunks, grad_chunk, (zero, zero))
    first = jnp.sum(one, axis=1, keepdims=True) / C
    second = jnp.sum(two, axis=1, keepdims=True) / C

    def conv_grad(cb, _):
        gext[cb, pl.ds(0, T), :] = (gc[cb] - first - cen[cb] * second) * inv
        return _

    lax.fori_loop(0, chunks, conv_grad, 0)
    send(gext.at[:, pl.ds(0, HB), :], gext.at[:, pl.ds(T, HB), :], ids["back"], preceding, d)

    def taps_chunk(cb, _):
        for k in range(K):
            acc = jnp.zeros((8, LANES), f32)
            for rb in range(T // RB):
                prod = gext[cb, pl.ds(rb * RB, RB), :] * ext[cb, pl.ds(HB - k + rb * RB, RB), :]
                acc = acc + jnp.sum(prod.reshape(RB // 8, 8, LANES), axis=0)
            kg[cb, pl.ds(k, 1), :] = jnp.sum(acc, axis=0, keepdims=True)
        return _

    lax.fori_loop(0, chunks, taps_chunk, 0)
    for j in range(1, S):
        to = lax.rem(s + j, S)
        send(kg.at[pl.ds(to * cps, cps)], krecv.at[j], ids["kg"] + j, to, d)
    send_blocks(S // 2, S)

    arrived(gext.at[:, pl.ds(T, HB), :], ids["back"])

    @pl.when(s == S - 1)
    def _():
        gext[:, pl.ds(T, HB), :] = jnp.zeros((chunks, HB, LANES), f32)

    def gated_chunk(cb, _):
        cols = pl.ds(pl.multiple_of(cb * LANES, LANES), LANES)
        tf = kall[cb].astype(f32)
        for rb in range(T // RB):
            rows = pl.ds(rb * RB, RB)
            acc = jnp.zeros((RB, LANES), f32)
            for k in range(K):
                acc = acc + tf[k : k + 1] * gext[cb, pl.ds(k + rb * RB, RB), :]
            acc = acc.astype(bf16).astype(f32)
            sig = jax.nn.sigmoid(gate[rows, cols].astype(f32))
            gv[rows, cols] = (acc * sig).astype(bf16)
            gg[rows, cols] = (acc * val[rows, cols].astype(f32) * sig * (1.0 - sig)).astype(bf16)
        return _

    lax.fori_loop(0, chunks, gated_chunk, 0)

    acc = kg[pl.ds(s * cps, cps)]
    for j in range(1, S):
        arrived(krecv.at[j], ids["kg"] + j)
        acc = acc + krecv[j]
    ksum[...] = acc
    for j in range(1, N):
        send(ksum, k2recv.at[j], ids["k2"] + j, s, lax.rem(d + j, N))
    for j in range(1, N):
        arrived(k2recv.at[j], ids["k2"] + j)
        acc = acc + k2recv[j]
    for c in range(cps):
        cols = slice(c * LANES, (c + 1) * LANES)
        kout[:, cols] = (acc[c] * factor)[:K]
        gout[:, cols] = (acc[c] * factor)[K : K + 1]

    home = me // S
    for q in range(S):
        @pl.when(jnp.logical_or(q != s, home != d))
        def _():
            arrived(rbuf.at[q], ids["rs"] + q)

    def sum_tile(n, _):
        cols = pl.ds(pl.multiple_of(n * LANES, LANES), LANES)
        acc = rbuf[0, :, cols].astype(f32)
        for q in range(1, S):
            acc = acc + rbuf[q, :, cols].astype(f32)
        gw[:, cols] = acc * factor
        return _

    lax.fori_loop(0, chunks, sum_tile, 0)
    for j in range(S):
        owner, rows, c = block_of(j)

        @pl.when(owner != me)
        def _():
            c.wait_send()

    for c in waits:
        c.wait_send()


def shards(out_cotangent, value_pre, gate_pre, out_weight, conv_kernel, norm_gain):
    S, N = lax.axis_size("sp"), lax.axis_size("dp")
    _, T, C = out_cotangent.shape
    K = conv_kernel.shape[0]
    chunks, cps, cpd, block = C // LANES, C // LANES // S, C // LANES // N, C // (S * N)
    HB = -(-(K - 1) // 16) * 16
    KP = -(-(K + 1) // 16) * 16
    packed = jnp.concatenate(
        [conv_kernel, norm_gain[None], jnp.zeros((KP - K - 1, C // S), bf16)], axis=0
    )
    packed = jnp.transpose(packed.reshape(KP, cps, LANES), (1, 0, 2))
    ids, count = {}, 0
    for name, size in (
        ("taps", S), ("front", 1), ("back", 1), ("partner", 1), ("mirror", N // 2 * HALVES),
        ("relay", N // 2 * HALVES), ("act", N), ("ga", N), ("rs", S), ("kg", S), ("k2", N),
    ):
        ids[name] = count
        count += size
    vm = pl.BlockSpec(memory_space=pltpu.VMEM)
    grad_value, grad_gate, grad_weight, grad_taps, grad_gain = pl.pallas_call(
        functools.partial(block_kernel, S, N, T, C, K, HB, ids),
        out_shape=(
            jax.ShapeDtypeStruct((T, C), bf16),
            jax.ShapeDtypeStruct((T, C), bf16),
            jax.ShapeDtypeStruct((block, C), f32),
            jax.ShapeDtypeStruct((K, C // S), f32),
            jax.ShapeDtypeStruct((1, C // S), f32),
        ),
        in_specs=[vm] * 5,
        out_specs=(vm,) * 5,
        scratch_shapes=[
            pltpu.VMEM((N, T, C), bf16),
            pltpu.VMEM((chunks, T + HB, LANES), f32),
            pltpu.VMEM((chunks, T, LANES), f32),
            pltpu.VMEM((chunks, T, LANES), f32),
            pltpu.VMEM((chunks, T + HB, LANES), f32),
            pltpu.VMEM((chunks, KP, LANES), bf16),
            pltpu.VMEM((chunks, T, LANES), bf16),
            pltpu.VMEM((N, cpd, T, LANES), bf16),
            pltpu.VMEM((N, cpd, T, LANES), bf16),
            pltpu.VMEM((chunks, T, LANES), bf16),
            pltpu.VMEM((cpd * LANES, C), bf16),
            pltpu.VMEM((S, block, C), bf16),
            pltpu.VMEM((chunks, KP, LANES), f32),
            pltpu.VMEM((S, cps, KP, LANES), f32),
            pltpu.VMEM((cps, KP, LANES), f32),
            pltpu.VMEM((N, cps, KP, LANES), f32),
            pltpu.SemaphoreType.DMA((count,)),
            pltpu.SemaphoreType.DMA((count,)),
        ],
        compiler_params=pltpu.CompilerParams(
            collective_id=0, has_side_effects=True, vmem_limit_bytes=60 * 1024 * 1024
        ),
        name="block_backward",
    )(out_cotangent[0], value_pre[0], gate_pre[0], out_weight, packed)
    return grad_value[None], grad_gate[None], grad_weight, grad_taps, grad_gain[0]


def solution(mesh):
    placed = (
        P("dp", "sp", None),
        P("dp", "sp", None),
        P("dp", "sp", None),
        P("dp", None),
        P(None, "sp"),
        P("sp"),
    )
    return jax.shard_map(
        shards,
        mesh=mesh,
        in_specs=placed,
        out_specs=(
            P("dp", "sp", None),
            P("dp", "sp", None),
            P(("sp", "dp"), None),
            P(None, "sp"),
            P("sp"),
        ),
        check_vma=False,
    )
```
